32 devices in a mesh: fs: 8 (over z, y), tp: 4 (over x, core).
Axes of the slice: x: 2, y: 2, z: 4, core: 2. Of those that a mesh axis runs over, the one named last changes fastest.
Arguments:
- tokens: bfloat16 [640, 3072], P('tp'), may hold values from -6 to 6
- gain_first: float32 [3072], replicated, may hold values from 0.1 to 1.9
- gain_second: float32 [3072], replicated, may hold values from 0.1 to 1.9
- gate_first: float32 [3072, 8192], P('fs', 'tp'), may hold values from -0.109375 to 0.109375
- up_first: float32 [3072, 8192], P('fs', 'tp'), may hold values from -0.109375 to 0.109375
- down_first: float32 [8192, 3072], P('fs', 'tp'), may hold values from -0.09375 to 0.09375
- gate_second: float32 [3072, 8192], P('fs', 'tp'), may hold values from -0.109375 to 0.109375
- up_second: float32 [3072, 8192], P('fs', 'tp'), may hold values from -0.109375 to 0.109375
- down_second: float32 [8192, 3072], P('fs', 'tp'), may hold values from -0.09375 to 0.09375
Outputs:
- result_rows: bfloat16 [640, 3072], P('tp')
- serve_gate_first: bfloat16 [3072, 8192], P(None, 'fs')
- serve_up_first: bfloat16 [3072, 8192], P(None, 'fs')
- serve_down_first: bfloat16 [8192, 3072], P('fs')
- serve_gate_second: bfloat16 [3072, 8192], P(None, 'fs')
- serve_up_second: bfloat16 [3072, 8192], P(None, 'fs')
- serve_down_second: bfloat16 [8192, 3072], P('fs')
The draws below stay inside these ranges and needn't reach their ends.
All inputs are finite; a program needn't handle non-finite values.
Results may differ from the reference program's by a relative error of at most 0.011.
Values may be sent and summed in bfloat16 or wider, within the bound.
No kernel may reach another device: no remote copies, remote signals or barrier semaphores. Data moves between devices by JAX's collectives and lax.ppermute only.
A program may use at most 192 MiB of HBM per device.

```python
import jax
import jax.numpy as jnp
from jax import lax

D = 3072
FF = 8192
TOKENS = 640


def with_spikes(drawn, own_key, source, target, shards_of, factor):
    def block_of(axis_at):
        return (jnp.arange(drawn.shape[axis_at]) // (drawn.shape[axis_at] // shards_of)).reshape((-1,) + (1,) * (drawn.ndim - 1 - axis_at))

    first = jax.random.permutation(own_key, shards_of)[block_of(target)]
    far = (block_of(target) + shards_of // 2) % shards_of
    return jnp.where((block_of(source) == first) | (block_of(source) == far), factor * drawn, drawn)


def level_of(stream_key, dims, split, smallest, largest):
    def one(dim, parts):
        draws = jax.random.uniform(jax.random.fold_in(jax.random.fold_in(stream_key, 6), dim), (parts,), jnp.float32, smallest / len(split), largest / len(split))
        return jnp.repeat(jnp.exp(draws), dims[dim] // parts).reshape((-1,) + (1,) * (len(dims) - dim - 1))

    level = one(*split[0])
    for cut in split[1:]:
        level = level * one(*cut)
    return level


def scatter_about(key, extent, deviation, most, shards=(), held_as=jnp.bfloat16):
    values = deviation * jax.random.normal(key, extent, jnp.float32)
    if shards:
        values = values * level_of(key, extent, shards, -0.22, 0.18)
    return jnp.clip(values, -most, most).astype(held_as)


def bell_draw_with(stream_key, dims, width, most, shards, heavy, kind=jnp.bfloat16):
    array = width * jax.random.normal(stream_key, dims, jnp.float32)
    if shards:
        array = array * level_of(stream_key, dims, shards, -0.22, 0.18)
    return jnp.clip(with_spikes(array, jax.random.fold_in(stream_key, 3), *heavy), -most, most).astype(kind)


def setup_inputs(seed: int = 0) -> dict:
    seeds = jax.random.split(jax.random.key(seed), 10)
    tokens = scatter_about(seeds[0], (TOKENS, D), 1.0, 6.0, ((0, 4),))
    gain_first = jnp.clip(1.0 + 0.18 * jax.random.normal(seeds[1], (D,), jnp.float32), 0.1, 1.9)
    gain_second = jnp.clip(1.0 + 0.18 * jax.random.normal(seeds[2], (D,), jnp.float32), 0.1, 1.9)
    gate_first = scatter_about(seeds[3], (D, FF), D ** -0.5, 0.109375, ((0, 8), (1, 4)), jnp.float32)
    up_first = scatter_about(seeds[4], (D, FF), D ** -0.5, 0.109375, ((0, 8), (1, 4)), jnp.float32)
    down_first = bell_draw_with(seeds[5], (FF, D), FF ** -0.5, 0.09375, ((0, 8), (1, 4)), (0, 1, 8, 2.0), jnp.float32)
    gate_second = scatter_about(seeds[6], (D, FF), D ** -0.5, 0.109375, ((0, 8), (1, 4)), jnp.float32)
    up_second = scatter_about(seeds[7], (D, FF), D ** -0.5, 0.109375, ((0, 8), (1, 4)), jnp.float32)
    down_second = bell_draw_with(seeds[8], (FF, D), FF ** -0.5, 0.09375, ((0, 8), (1, 4)), (0, 1, 8, 2.0), jnp.float32)
    return {"tokens": tokens, "gain_first": gain_first, "gain_second": gain_second, "gate_first": gate_first, "up_first": up_first, "down_first": down_first, "gate_second": gate_second, "up_second": up_second, "down_second": down_second}


def plain_norm(values):
    values = values.astype(jnp.float32)
    center = lax.optimization_barrier(jnp.mean(values, axis=-1, keepdims=True))
    spread = lax.optimization_barrier(jnp.mean(jnp.square(values - center), axis=-1, keepdims=True))
    return (values - center) * jax.lax.rsqrt(spread + 1e-05)

def fold_gain(weight, scales):
    return (scales[:, None] * weight).astype(jnp.bfloat16)

def half_step(normed, scales, w_gate, w_rising, w_down):
    gate_part = jnp.dot(normed, w_gate, preferred_element_type=jnp.float32)
    rising = jnp.dot(normed, w_rising, preferred_element_type=jnp.float32)
    hidden = (jax.nn.silu(gate_part) * rising).astype(jnp.bfloat16)
    block = jnp.dot(hidden, w_down, preferred_element_type=jnp.float32)
    mixed = 1.6817928 * scales[None, :] * normed.astype(jnp.float32) + 0.5 * block
    return plain_norm(mixed).astype(jnp.bfloat16)

def reference(tokens, gain_first, gain_second, gate_first, up_first, down_first, gate_second, up_second, down_second):
    serve_gate_first = fold_gain(gate_first, gain_first)
    serve_up_first = fold_gain(up_first, gain_first)
    serve_gate_second = fold_gain(gate_second, gain_second)
    serve_up_second = fold_gain(up_second, gain_second)
    serve_down_first = down_first.astype(jnp.bfloat16)
    serve_down_second = down_second.astype(jnp.bfloat16)
    normed_zero = plain_norm(tokens).astype(jnp.bfloat16)
    normed_one = half_step(normed_zero, gain_first, serve_gate_first, serve_up_first, serve_down_first)
    result_rows = half_step(normed_one, gain_second, serve_gate_second, serve_up_second, serve_down_second)
    return (result_rows, serve_gate_first, serve_up_first, serve_down_first, serve_gate_second, serve_up_second, serve_down_second)
```

```python
import functools

import jax
import jax.numpy as jnp
from jax import lax
from jax.experimental import pallas as pl
from jax.experimental.pallas import tpu as pltpu
from jax.sharding import PartitionSpec as P

LANES = 128


def plain_norm(values):
    values = values.astype(jnp.float32)
    center = jnp.mean(values, axis=-1, keepdims=True)
    spread = jnp.mean(jnp.square(values - center), axis=-1, keepdims=True)
    return (values - center) * lax.rsqrt(spread + 1e-05)


def swap(value, axis, size, mask):
    return lax.ppermute(value, axis, [(i, i ^ mask) for i in range(size)])


def place(parts, masks, own, rows_each, stacked=False):
    count = len(parts)
    rows, width = parts[0].shape
    shape = (count, rows, width) if stacked else (rows, count * width)

    def body(own_ref, *refs):
        target = refs[count]
        for k in range(count):
            slot = jnp.bitwise_xor(own_ref[0], masks[k])
            if stacked:
                target[slot] = refs[k][...]
            else:
                target[:, pl.ds(pl.multiple_of(slot * width, LANES), width)] = refs[k][...]

    out_block = (count, rows_each, width) if stacked else (rows_each, count * width)
    out_map = (lambda i, own_ref: (0, i, 0)) if stacked else (lambda i, own_ref: (i, 0))
    return pl.pallas_call(
        body,
        out_shape=jax.ShapeDtypeStruct(shape, parts[0].dtype),
        grid_spec=pltpu.PrefetchScalarGridSpec(
            num_scalar_prefetch=1,
            grid=(rows // rows_each,),
            in_specs=[pl.BlockSpec((rows_each, width), lambda i, own_ref: (i, 0))] * count,
            out_specs=pl.BlockSpec(out_block, out_map),
        ),
        cost_estimate=pl.CostEstimate(
            flops=4_000_000,
            transcendentals=0,
            bytes_accessed=4 * count * parts[0].size,
        ),
    )(own.reshape(1), *parts)


def hidden_of(normed, w_gate, w_rising):
    gate_part = jnp.dot(normed, w_gate, preferred_element_type=jnp.float32)
    rising = jnp.dot(normed, w_rising, preferred_element_type=jnp.float32)
    return (jax.nn.silu(gate_part) * rising).astype(jnp.bfloat16)


def on_device(
    fs_size,
    tp_size,
    tokens,
    gain_first,
    gain_second,
    gate_first,
    up_first,
    down_first,
    gate_second,
    up_second,
    down_second,
):
    fs_own = lax.axis_index("fs").astype(jnp.int32)
    tp_own = lax.axis_index("tp").astype(jnp.int32)
    rows, cols = gate_first.shape
    per = fs_size // tp_size
    block = cols // per
    half = tp_size // 2

    def fold_gain(weight, scales):
        picked = lax.dynamic_slice_in_dim(scales, fs_own * rows, rows, 0)
        return (picked[:, None] * weight).astype(jnp.bfloat16)

    def quarter_way(weight, scales):
        width = block // tp_size
        folded = fold_gain(weight, scales).reshape(rows, per, tp_size, width)

        def cut(mask):
            one = lax.dynamic_index_in_dim(folded, tp_own ^ mask, 2, keepdims=False)
            return one.transpose(1, 0, 2)

        arrived = [cut(0)] + [swap(cut(m), "tp", tp_size, m) for m in range(1, tp_size)]
        arrived = [a.reshape(per * rows, width) for a in arrived]
        lined = place(arrived, range(tp_size), tp_own, rows, stacked=True)
        lined = lined.reshape(fs_size, rows, width)
        mine = lax.all_to_all(lined, "fs", 0, 0, tiled=True)
        mine = mine.reshape(fs_size * rows, width)
        across = swap(mine, "tp", tp_size, half)
        return [mine, across, swap(mine, "tp", tp_size, 1), swap(across, "tp", tp_size, 1)]

    masks = [0, half, 1, half + 1]

    def down_way(weight):
        mine = weight.astype(jnp.bfloat16)
        across = swap(mine, "tp", tp_size, half)
        parts = [mine, across, swap(mine, "tp", tp_size, 1), swap(across, "tp", tp_size, 1)]
        return place(parts, masks, tp_own, 256)

    def finish(parts):
        return place(parts, masks, tp_own, 512)

    def step(normed, scales, w_gate, w_rising, w_down):
        hidden = hidden_of(normed, w_gate, w_rising)
        partial = jnp.dot(hidden, w_down, preferred_element_type=jnp.float32)
        share = normed.shape[0] // fs_size
        cut_rows = partial.astype(jnp.bfloat16).reshape(fs_size, share, -1)
        total = lax.dynamic_index_in_dim(
            partial.reshape(fs_size, share, -1), fs_own, 0, keepdims=False
        )
        for m in range(1, fs_size):
            sent = lax.dynamic_index_in_dim(cut_rows, fs_own ^ m, 0, keepdims=False)
            total = total + swap(sent, "fs", fs_size, m).astype(jnp.float32)
        own_rows = lax.dynamic_slice_in_dim(normed, fs_own * share, share, 0)
        mixed = 1.6817928 * scales[None, :] * own_rows.astype(jnp.float32) + 0.5 * total
        out = plain_norm(mixed).astype(jnp.bfloat16)
        pieces = [out] + [swap(out, "fs", fs_size, m) for m in range(1, fs_size)]
        joined = place(pieces, range(fs_size), fs_own, share, stacked=True)
        return joined.reshape(normed.shape)

    serve_gate_first = finish(quarter_way(gate_first, gain_first))
    serve_up_first = finish(quarter_way(up_first, gain_first))
    serve_down_first = down_way(down_first)
    serve_gate_second = finish(quarter_way(gate_second, gain_second))
    serve_up_second = finish(quarter_way(up_second, gain_second))
    serve_down_second = down_way(down_second)
    normed_zero = plain_norm(tokens).astype(jnp.bfloat16)
    normed_one = step(
        normed_zero, gain_first, serve_gate_first, serve_up_first, serve_down_first
    )
    result_rows = step(
        normed_one, gain_second, serve_gate_second, serve_up_second, serve_down_second
    )
    return (
        result_rows,
        serve_gate_first,
        serve_up_first,
        serve_down_first,
        serve_gate_second,
        serve_up_second,
        serve_down_second,
    )


def half_step(normed, scales, w_gate, w_rising, w_down):
    gate_part = jnp.dot(normed, w_gate, preferred_element_type=jnp.float32)
    rising = jnp.dot(normed, w_rising, preferred_element_type=jnp.float32)
    hidden = (jax.nn.silu(gate_part) * rising).astype(jnp.bfloat16)
    partial_value = jnp.dot(hidden, w_down, preferred_element_type=jnp.float32)
    block = lax.psum(partial_value, "fs")
    mixed = 1.6817928 * scales[None, :] * normed.astype(jnp.float32) + 0.5 * block
    return plain_norm(mixed).astype(jnp.bfloat16)


def on_device_plain(
    tokens,
    gain_first,
    gain_second,
    gate_first,
    up_first,
    down_first,
    gate_second,
    up_second,
    down_second,
):
    row_count = gate_first.shape[0]
    offset = lax.axis_index("fs") * row_count

    def fold_gain(weight, scales):
        picked = lax.dynamic_slice_in_dim(scales, offset, row_count, 0)
        return (picked[:, None] * weight).astype(jnp.bfloat16)

    widened = (
        lax.all_gather(fold_gain(gate_first, gain_first), "tp", axis=1, tiled=True),
        lax.all_gather(fold_gain(up_first, gain_first), "tp", axis=1, tiled=True),
        lax.all_gather(fold_gain(gate_second, gain_second), "tp", axis=1, tiled=True),
        lax.all_gather(fold_gain(up_second, gain_second), "tp", axis=1, tiled=True),
        lax.all_gather(down_first.astype(jnp.bfloat16), "tp", axis=1, tiled=True),
        lax.all_gather(down_second.astype(jnp.bfloat16), "tp", axis=1, tiled=True),
    )
    regrouped = (
        lax.all_to_all(widened[0], "fs", split_axis=1, concat_axis=0, tiled=True),
        lax.all_to_all(widened[1], "fs", split_axis=1, concat_axis=0, tiled=True),
        lax.all_to_all(widened[2], "fs", split_axis=1, concat_axis=0, tiled=True),
        lax.all_to_all(widened[3], "fs", split_axis=1, concat_axis=0, tiled=True),
    )
    serve_gate_first, serve_up_first, serve_gate_second, serve_up_second = regrouped
    serve_down_first = widened[4]
    serve_down_second = widened[5]
    normed_zero = plain_norm(tokens).astype(jnp.bfloat16)
    normed_one = half_step(
        normed_zero, gain_first, serve_gate_first, serve_up_first, serve_down_first
    )
    result_rows = half_step(
        normed_one, gain_second, serve_gate_second, serve_up_second, serve_down_second
    )
    return (
        result_rows,
        serve_gate_first,
        serve_up_first,
        serve_down_first,
        serve_gate_second,
        serve_up_second,
        serve_down_second,
    )


def solution(mesh):
    placed = (
        P("tp", None),
        P(),
        P(),
        P("fs", "tp"),
        P("fs", "tp"),
        P("fs", "tp"),
        P("fs", "tp"),
        P("fs", "tp"),
        P("fs", "tp"),
    )
    fs_size, tp_size = mesh.shape["fs"], mesh.shape["tp"]

    def body(*args):
        rows, cols = args[3].shape
        down_cols = args[5].shape[1]
        fits = (
            tp_size == 4
            and fs_size == 8
            and cols * tp_size % (fs_size * tp_size * LANES) == 0
            and down_cols % LANES == 0
            and args[0].shape[0] % fs_size == 0
        )
        if not fits:
            return on_device_plain(*args)
        return on_device(fs_size, tp_size, *args)

    return jax.shard_map(
        body,
        mesh=mesh,
        in_specs=placed,
        out_specs=(
            P("tp", None),
            P(None, "fs"),
            P(None, "fs"),
            P("fs", None),
            P(None, "fs"),
            P(None, "fs"),
            P("fs", None),
        ),
        check_vma=False,
    )
```
